32 devices in a mesh: sp: 16 (over z, y, x), tp: 2 (over core).
Axes of the slice: x: 2, y: 2, z: 4, core: 2. Of those that a mesh axis runs over, the one named last changes fastest.
Arguments:
- resid: bfloat16 [6144, 2048], P('sp'), may hold values from -6 to 6
- x_branch: bfloat16 [6144, 2048], P('sp', 'tp'), may hold values from -6 to 6
- gate_branch: bfloat16 [6144, 2048], P('sp', 'tp'), may hold values from -6 to 6
- conv_w: float32 [4, 2048], P(None, 'tp'), may hold values from -3 to 3
- gate_a_w: bfloat16 [32, 64, 64], P('tp'), may hold values from -0.75 to 0.75
- gate_x_w: bfloat16 [32, 64, 64], P('tp'), may hold values from -0.75 to 0.75
- decay_rate: float32 [2048], P('tp'), may hold values from 0 to 0.01, as said below
- decay_extra: float32 [6144, 2048], P('sp', 'tp'), may hold values from -3 to 0, as said below
- w_proj: bfloat16 [2048, 2048], P('tp'), may hold values from -0.125 to 0.125
- mix_gain: float32 [2048], replicated, may hold values from 0.1 to 1.9
- pre_gain: float32 [2048], replicated, may hold values from 0.1 to 1.9
- w_gate: bfloat16 [2048, 5632], P('sp', 'tp'), may hold values from -0.125 to 0.125
- w_up: bfloat16 [2048, 5632], P('sp', 'tp'), may hold values from -0.125 to 0.125
- w_down: bfloat16 [5632, 2048], P('tp', 'sp'), may hold values from -0.078125 to 0.078125
- out_gain: float32 [2048], replicated, may hold values from 0.1 to 1.9
Outputs:
- stream_out: bfloat16 [6144, 2048], P(('sp', 'tp'))
The draws below stay inside these ranges and needn't reach their ends.
Inputs may be any that keep to these rules, and one draw needn't show every extreme that they name: `decay_rate`: positive rates. `decay_extra`: non-positive values.
All inputs are finite; a program needn't handle non-finite values.
Results may differ from the reference program's by a relative error of at most 0.015.
Values may be sent and summed in bfloat16 or wider, within the bound.
No kernel may reach another device: no remote copies, remote signals or barrier semaphores. Data moves between devices by JAX's collectives and lax.ppermute only.
A program may use at most 128 MiB of HBM per device.

```python
import math
import jax
import jax.numpy as jnp
from jax import lax

D = 2048
BLOCKS = 32
BW = 64
RECURRENCE_WIDTH = 2048
FF = 5632
CONV = 4
TOK_DEV = 384
TOKEN_SLOTS = 6144
N_TP = 2


def draw_decay_rate(key, part):
    key_pick, key_fast, key_slow = jax.random.split(key, 3)
    fast_share = 0.5
    is_fast = jax.random.uniform(key_pick, (RECURRENCE_WIDTH,), jnp.float32) < fast_share
    fast_rate = jnp.exp(jax.random.uniform(key_fast, (RECURRENCE_WIDTH,), jnp.float32, minval=math.log(1.0 / 240.0), maxval=math.log(1.0 / 120.0)))
    slow_rate = math.log(10.0) / (16.0 * TOKEN_SLOTS) * jax.random.uniform(key_slow, (RECURRENCE_WIDTH,), jnp.float32, minval=0.25, maxval=1.0)
    return jnp.where(is_fast, fast_rate, slow_rate).astype(jnp.float32)


def draw_decay_extra(key, part):
    key_level, key_location_draw, key_extent_draw = jax.random.split(key, 3)
    nblocks = TOKEN_SLOTS // TOK_DEV
    levels = jax.random.uniform(key_level, (nblocks, RECURRENCE_WIDTH), jnp.float32) * (-0.5 / TOKEN_SLOTS)
    drawn_regime = jnp.repeat(levels, TOK_DEV, axis=0)
    spike_token_rows = jax.random.randint(key_location_draw, (3,), 0, TOKEN_SLOTS)
    spike_extent = jax.random.uniform(key_extent_draw, (3, RECURRENCE_WIDTH), jnp.float32, minval=math.log(0.5), maxval=math.log(0.8))
    token_offsets = jnp.arange(TOKEN_SLOTS)
    inside_spike = (token_offsets[:, None] == spike_token_rows[None, :]).astype(jnp.float32)
    return (drawn_regime + jnp.dot(inside_spike, spike_extent)).astype(jnp.float32)


def block_scale(own_key, extent, cuts, least, largest):
    factor_of = 1.0
    for axis_at, parts in cuts:
        steps = jax.random.uniform(jax.random.fold_in(jax.random.fold_in(own_key, 6), axis_at), (parts,), jnp.float32, least / len(cuts), largest / len(cuts))
        factor_of = factor_of * jnp.repeat(jnp.exp(steps), extent[axis_at] // parts).reshape((-1,) + (1,) * (len(extent) - 1 - axis_at))
    return factor_of


def bell_draw(key, dims, width, reach, shards=(), held_as=jnp.bfloat16):
    array = width * jax.random.normal(key, dims, jnp.float32)
    if shards:
        array = array * block_scale(key, dims, shards, -0.22, 0.18)
    return jnp.clip(array, -reach, reach).astype(held_as)


def setup_inputs(seed: int = 0) -> dict:
    seeds = jax.random.split(jax.random.key(seed), 16)
    return {
        "resid": bell_draw(seeds[0], (TOKEN_SLOTS, D), 1.0, 6.0, ((0, 16),)),
        "x_branch": bell_draw(seeds[1], (TOKEN_SLOTS, RECURRENCE_WIDTH), 1.0, 6.0, ((0, 16), (1, 2))),
        "gate_branch": bell_draw(seeds[2], (TOKEN_SLOTS, RECURRENCE_WIDTH), 1.0, 6.0, ((0, 16), (1, 2))),
        "conv_w": bell_draw(seeds[3], (CONV, RECURRENCE_WIDTH), CONV ** -0.5, 3.0, ((1, 2),), jnp.float32),
        "gate_a_w": bell_draw(seeds[4], (BLOCKS, BW, BW), BW ** -0.5, 0.75, ((0, 2),)),
        "gate_x_w": bell_draw(seeds[5], (BLOCKS, BW, BW), BW ** -0.5, 0.75, ((0, 2),)),
        "decay_rate": draw_decay_rate(jax.random.fold_in(seeds[15], 71), 0),
        "decay_extra": draw_decay_extra(jax.random.fold_in(seeds[15], 71), 0),
        "w_proj": bell_draw(seeds[8], (RECURRENCE_WIDTH, D), RECURRENCE_WIDTH ** -0.5, 0.125, ((0, 2),)),
        "mix_gain": jnp.clip(1.0 + 0.18 * jax.random.normal(seeds[9], (D,), jnp.float32), 0.1, 1.9),
        "pre_gain": jnp.clip(1.0 + 0.18 * jax.random.normal(seeds[10], (D,), jnp.float32), 0.1, 1.9),
        "w_gate": bell_draw(seeds[11], (D, FF), D ** -0.5, 0.125, ((0, 16), (1, 2))),
        "w_up": bell_draw(seeds[12], (D, FF), D ** -0.5, 0.125, ((0, 16), (1, 2))),
        "w_down": bell_draw(seeds[13], (FF, D), FF ** -0.5, 0.078125, ((0, 2), (1, 16))),
        "out_gain": jnp.clip(1.0 + 0.18 * jax.random.normal(seeds[14], (D,), jnp.float32), 0.1, 1.9),
    }


LRU_SCALE = 8.0
NORM_EPS = 1e-06

def chain(earlier, later):
    return (earlier[0] * later[0], later[0] * earlier[1] + later[1])

def rms_scale(values, gains):
    return values * lax.rsqrt(lax.optimization_barrier(jnp.mean(values * values, axis=-1, keepdims=True)) + NORM_EPS) * gains

def reference(resid, x_branch, gate_branch, conv_w, gate_a_w, gate_x_w, decay_rate, decay_extra, w_proj, mix_gain, pre_gain, w_gate, w_up, w_down, out_gain):
    padded = jnp.pad(x_branch.astype(jnp.float32), ((CONV - 1, 0), (0, 0)))
    conv = padded[0:TOKEN_SLOTS] * conv_w[0]
    for tap in range(1, CONV):
        conv = conv + padded[tap:tap + TOKEN_SLOTS] * conv_w[tap]
    conv_out = conv.astype(jnp.bfloat16)
    grouped = conv_out.astype(jnp.float32).reshape(TOKEN_SLOTS, BLOCKS, BW)
    recur = jax.nn.sigmoid(jnp.einsum('rnc,ncd->rnd', grouped, gate_a_w.astype(jnp.float32)).reshape(TOKEN_SLOTS, RECURRENCE_WIDTH))
    inject = jax.nn.sigmoid(jnp.einsum('rnc,ncd->rnd', grouped, gate_x_w.astype(jnp.float32)).reshape(TOKEN_SLOTS, RECURRENCE_WIDTH))
    log_decay = -LRU_SCALE * recur * decay_rate + decay_extra
    decay = jnp.exp(log_decay)
    drive = jnp.sqrt(-jnp.expm1(2.0 * log_decay)) * inject * conv_out.astype(jnp.float32)
    _, state = lax.associative_scan(chain, (decay, drive), axis=0)
    mixer = (state * jax.nn.gelu(gate_branch.astype(jnp.float32))).astype(jnp.bfloat16)
    group_w = RECURRENCE_WIDTH // N_TP
    mixed = jnp.zeros((TOKEN_SLOTS, D), jnp.float32)
    for group in range(N_TP):
        partial_sum = jnp.dot(mixer[:, group * group_w:(group + 1) * group_w], w_proj[group * group_w:(group + 1) * group_w], preferred_element_type=jnp.float32)
        mixed = mixed + lax.optimization_barrier(partial_sum.astype(jnp.bfloat16)).astype(jnp.float32)
    stream = resid.astype(jnp.float32) + rms_scale(mixed, mix_gain)
    normed = rms_scale(stream, pre_gain).astype(jnp.bfloat16)
    group_f = FF // N_TP
    ffn = jnp.zeros((TOKEN_SLOTS, D), jnp.float32)
    for group in range(N_TP):
        gate = jnp.dot(normed, w_gate[:, group * group_f:(group + 1) * group_f], preferred_element_type=jnp.float32)
        upward = jnp.dot(normed, w_up[:, group * group_f:(group + 1) * group_f], preferred_element_type=jnp.float32)
        hidden = (jax.nn.silu(gate) * upward).astype(jnp.bfloat16)
        partial_sum = jnp.dot(hidden, w_down[group * group_f:(group + 1) * group_f], preferred_element_type=jnp.float32)
        ffn = ffn + lax.optimization_barrier(partial_sum.astype(jnp.bfloat16)).astype(jnp.float32)
    return (stream + 0.5 * rms_scale(ffn, out_gain)).astype(jnp.bfloat16)
```

```python
import jax
import jax.numpy as jnp
from jax import lax
from jax.experimental import pallas as pl
from jax.experimental.pallas import tpu as pltpu
from jax.sharding import Mesh, PartitionSpec as P

LRU_SCALE = 8.0
NORM_EPS = 1e-06


def chain(earlier, later):
    return (earlier[0] * later[0], later[0] * earlier[1] + later[1])


def rms_scale(values, gains):
    return values * lax.rsqrt(jnp.mean(values * values, axis=-1, keepdims=True) + NORM_EPS) * gains


def one_minus_exp(y):
    series = 1.0
    for n in (8, 7, 6, 5, 4, 3, 2):
        series = 1.0 + y * (1.0 / n) * series
    return jnp.where(y > -0.35, -y * series, 1.0 - jnp.exp(y))


def rows_down(a, k, fill, row):
    if k % 8 == 0:
        return jnp.concatenate([jnp.full((k, a.shape[1]), fill, a.dtype), a[:-k]], axis=0)
    return jnp.where(row >= k, pltpu.roll(a, k, 0), fill)


def recur_kernel(x, before, gate, taps, wa, wx, rate, extra, u_out, v_out, last_out):
    length, lanes = x.shape
    ntaps = taps.shape[0]
    row = lax.broadcasted_iota(jnp.int32, (length, lanes), 0)
    xf = x[...].astype(jnp.float32)
    prev = before[...].astype(jnp.float32)
    conv = None
    for tap in range(ntaps):
        k = ntaps - 1 - tap
        moved = xf
        if k:
            moved = pltpu.roll(xf, k, 0)
            for r in range(k):
                at = prev.shape[0] - k + r
                moved = jnp.where(row == r, prev[at : at + 1], moved)
        term = moved * taps[tap : tap + 1]
        conv = term if conv is None else conv + term
    conv_out = conv.astype(jnp.bfloat16)
    recur = 1.0 / (1.0 + jnp.exp(-jnp.dot(conv_out, wa[0], preferred_element_type=jnp.float32)))
    inject = 1.0 / (1.0 + jnp.exp(-jnp.dot(conv_out, wx[0], preferred_element_type=jnp.float32)))
    log_decay = -LRU_SCALE * recur * rate[...] + extra[...]
    decay = jnp.exp(log_decay)
    left = one_minus_exp(2.0 * log_decay)
    root = jnp.where(left > 0.0, left * lax.rsqrt(left), 0.0)
    drive = root * inject * conv_out.astype(jnp.float32)
    k = 1
    while k < length:
        drive = drive + decay * rows_down(drive, k, 0.0, row)
        decay = decay * rows_down(decay, k, 1.0, row)
        k *= 2
    g = jax.nn.gelu(gate[...].astype(jnp.float32))
    u_out[...] = drive * g
    v_out[...] = decay * g
    last_out[0:1] = decay[length - 1 : length]
    last_out[1:2] = drive[length - 1 : length]


def pair_blocks(w, per):
    n, b, _ = w.shape
    eye = jnp.eye(per, dtype=w.dtype)
    wide = w.reshape(n // per, per, b, 1, b) * eye[None, :, None, :, None]
    return wide.reshape(n // per, per * b, per * b)


def recurrence(x, before, gate, taps, wa, wx, rate, extra):
    length, width = x.shape
    b = wa.shape[1]
    per = max(1, min(128, width) // b)
    lanes = per * b
    col = lambda i: (0, i)
    blk = lambda i: (i, 0, 0)
    return pl.pallas_call(
        recur_kernel,
        grid=(width // lanes,),
        in_specs=[
            pl.BlockSpec((length, lanes), col),
            pl.BlockSpec((before.shape[0], lanes), col),
            pl.BlockSpec((length, lanes), col),
            pl.BlockSpec((taps.shape[0], lanes), col),
            pl.BlockSpec((1, lanes, lanes), blk),
            pl.BlockSpec((1, lanes, lanes), blk),
            pl.BlockSpec((1, lanes), col),
            pl.BlockSpec((length, lanes), col),
        ],
        out_specs=[
            pl.BlockSpec((length, lanes), col),
            pl.BlockSpec((length, lanes), col),
            pl.BlockSpec((2, lanes), col),
        ],
        out_shape=[
            jax.ShapeDtypeStruct((length, width), jnp.float32),
            jax.ShapeDtypeStruct((length, width), jnp.float32),
            jax.ShapeDtypeStruct((2, width), jnp.float32),
        ],
        compiler_params=pltpu.CompilerParams(dimension_semantics=("arbitrary",)),
        name="recurrence",
    )(x, before, gate, taps, pair_blocks(wa, per), pair_blocks(wx, per), rate[None], extra)


def turn(value, axis, k):
    n = lax.axis_size(axis)
    return lax.ppermute(value, axis, [(s, (s + k) % n) for s in range(n)])


def exclusive(part, axis):
    place = lax.axis_index(axis)
    none = jnp.stack([jnp.ones_like(part[0]), jnp.zeros_like(part[1])])
    got = none
    n = lax.axis_size(axis)
    sent = [(k, turn(part, axis, k)) for k in range(1, n)]
    for k, p in reversed(sent):
        p = jnp.where(place >= k, p, none)
        got = jnp.stack(chain(got, p))
    return got


def from_peers(part, halves):
    if halves == 2:
        rows = part.shape[0] // 2
        return part[:rows].astype(jnp.float32) + turn(part[rows:], "tp", 1).astype(jnp.float32)
    return lax.psum_scatter(part, "tp", scatter_dimension=0, tiled=True).astype(jnp.float32)


def with_peers(own, halves):
    if halves == 2:
        return jnp.concatenate([own, turn(own, "tp", 1)], axis=0)
    return lax.all_gather(own, "tp", axis=0, tiled=True)


def exchange(pieces, place, n):
    got = jnp.stack(
        [
            lax.dynamic_index_in_dim(pieces, place, 0, False)
            if k == 0
            else turn(lax.dynamic_index_in_dim(pieces, (place + k) % n, 0, False), "so", k)
            for k in range(n)
        ]
    )
    order = (place - jnp.arange(n)) % n
    return jnp.take(got, order, axis=0)


def shards(
    resid,
    x_branch,
    gate_branch,
    conv_w,
    gate_a_w,
    gate_x_w,
    decay_rate,
    decay_extra,
    w_proj,
    mix_gain,
    pre_gain,
    w_gate,
    w_up,
    w_down,
    out_gain,
):
    no, ni, nt = (lax.axis_size(a) for a in ("so", "si", "tp"))
    o, t = lax.axis_index("so"), lax.axis_index("tp")
    length = x_branch.shape[0]
    taps = conv_w.shape[0]
    share = length // nt
    width = resid.shape[1]

    r, f = w_gate.shape
    fs = f // no
    cut = jnp.stack([w_gate.reshape(r, no, fs), w_up.reshape(r, no, fs)], axis=2)
    cut = cut.reshape(r, no, 2 * fs).transpose(1, 0, 2)
    wide = exchange(cut, o, no).reshape(no * r, 2 * fs)
    wide = lax.all_gather(wide, "si", axis=0, tiled=True)
    tall = exchange(w_down.reshape(no, fs, r), o, no).reshape(no * fs, r)
    tall = lax.all_gather(tall, "si", axis=0, tiled=True)
    tall = tall.reshape(ni, no, fs, r).transpose(2, 1, 0, 3).reshape(fs, width)

    n_sp = no * ni
    before = lax.ppermute(
        x_branch[length - (taps - 1) :], ("so", "si"), [(s, s + 1) for s in range(n_sp - 1)]
    )
    u, v, last = recurrence(
        x_branch, before, gate_branch, conv_w, gate_a_w, gate_x_w, decay_rate, decay_extra
    )
    inner = exclusive(last, "si")
    whole = jnp.stack(chain(inner, last))
    total = jnp.where(lax.axis_index("si") == ni - 1, whole, 0.0)
    total = sum([total] + [turn(total, "si", k) for k in range(1, ni)])
    outer = exclusive(total, "so")
    carried = chain(outer, inner)[1]
    mixer = (u + v * carried[None, :]).astype(jnp.bfloat16)
    part = jnp.dot(mixer, w_proj, preferred_element_type=jnp.float32).astype(jnp.bfloat16)
    if nt == 2:
        part = part.reshape(2, share, width)
        part = jnp.concatenate(
            [lax.dynamic_index_in_dim(part, t, 0, False), lax.dynamic_index_in_dim(part, 1 - t, 0, False)]
        )
    mixed = from_peers(part, nt)
    own = lax.dynamic_slice_in_dim(resid, t * share, share, 0).astype(jnp.float32)
    stream = own + rms_scale(mixed, mix_gain)
    normed = rms_scale(stream, pre_gain).astype(jnp.bfloat16)
    normed = normed.reshape(share, no, ni, r).transpose(0, 2, 1, 3).reshape(share, width)

    def forward(rows):
        both = jnp.dot(rows, wide, preferred_element_type=jnp.float32)
        hidden = (jax.nn.silu(both[:, :fs]) * both[:, fs:]).astype(jnp.bfloat16)
        return jnp.dot(hidden, tall, preferred_element_type=jnp.float32).astype(jnp.bfloat16)

    order = sorted(range(no), key=lambda k: -min(k, no - k))
    rows = {k: with_peers(turn(normed, "so", k) if k else normed, nt) for k in order}
    ffn = None
    for k in order:
        piece = from_peers(forward(rows[k]), nt)
        if k:
            piece = turn(piece.astype(jnp.bfloat16), "so", no - k).astype(jnp.float32)
        ffn = piece if ffn is None else ffn + piece
    return (stream + 0.5 * rms_scale(ffn, out_gain)).astype(jnp.bfloat16)


def solution(mesh):
    n_sp, n_tp = mesh.shape["sp"], mesh.shape["tp"]
    inner = next(k for k in (4, 2, 1) if n_sp % k == 0)
    cut = Mesh(mesh.devices.reshape(n_sp // inner, inner, n_tp), ("so", "si", "tp"))
    sp = ("so", "si")
    return jax.shard_map(
        shards,
        mesh=cut,
        in_specs=(
            P(sp, None),
            P(sp, "tp"),
            P(sp, "tp"),
            P(None, "tp"),
            P("tp", None, None),
            P("tp", None, None),
            P("tp"),
            P(sp, "tp"),
            P("tp", None),
            P(),
            P(),
            P(sp, "tp"),
            P(sp, "tp"),
            P("tp", sp),
            P(),
        ),
        out_specs=P(("so", "si", "tp"), None),
        check_vma=False,
    )
```
